32 devices in a mesh: sp: 8 (over z, x), tp: 4 (over y, core).
Axes of the slice: x: 2, y: 2, z: 4, core: 2. Of those that a mesh axis runs over, the one named last changes fastest.
Arguments:
- tokens: bfloat16 [4096, 4096], P('sp'), may hold values from -6 to 6
- norm_gain: float32 [4096], replicated, may hold values from 0.1 to 1.9
- w_pool_in: bfloat16 [4096, 2048], P(None, 'tp'), may hold values from -0.09375 to 0.09375
- w_query: bfloat16 [4096, 2048], P(None, 'tp'), may hold values from -0.15625 to 0.15625
- w_key: bfloat16 [4096, 2048], P(None, 'tp'), may hold values from -0.15625 to 0.15625
- w_value: bfloat16 [4096, 2048], P(None, 'tp'), may hold values from -0.09375 to 0.09375
- pool_mix: bfloat16 [32, 64, 64], P('tp'), may hold values from -0.75 to 0.75
- pool_scale: float32 [2048], P('tp'), may hold values from 0.1 to 1.9
- lam: float32 [16], P('tp'), may hold values from 0.3 to 0.8
- head_gain: float32 [128], replicated, may hold values from 0.1 to 1.9
- pool_proj: bfloat16 [2048, 4096], P('tp'), may hold values from -0.125 to 0.125
- attn_proj: bfloat16 [2048, 4096], P('tp'), may hold values from -0.125 to 0.125
Outputs:
- mixed: bfloat16 [4096, 4096], P(('sp', 'tp'))
The draws below stay inside these ranges and needn't reach their ends.
All inputs are finite; a program needn't handle non-finite values.
Results may differ from the reference program's by a relative error of at most 0.015.
Values may be sent and summed in bfloat16 or wider, within the bound.
A program may use at most 128 MiB of HBM per device.

```python
import jax
import jax.numpy as jnp
from jax import lax

D = 4096
GROUPS = 32
GDIM = 64
HEADS = 16
HEAD = 64
VDIM = 128
SEGMENT = 64
REACH = 16
POOL = 2048
TOKENS = 4096
N_TP = 4


def weight_noise(key, stream_id):
    drawn = 1.3 * jax.random.normal(jax.random.fold_in(key, stream_id), (D, HEADS * 2 * HEAD), jnp.float32)
    return jnp.clip(drawn, -7.8, 7.8) * D ** (-0.5)


def draw_tokens(key, part):
    noise_key = jax.random.fold_in(key, 11)
    drawn = jax.random.normal(noise_key, (TOKENS, D), jnp.float32)
    return jnp.clip(drawn, -6.0, 6.0).astype(jnp.bfloat16)


def draw_w_query(key, part):
    noise_part = weight_noise(key, 21)
    drawn = noise_part
    return drawn.astype(jnp.bfloat16)


def draw_w_key(key, part):
    noise_part = weight_noise(key, 22)
    drawn = noise_part
    return drawn.astype(jnp.bfloat16)


def shard_levels(rng, shape, split, smallest, largest):
    level = 1.0
    for axis_at, shards_of in split:
        heights = jax.random.uniform(jax.random.fold_in(jax.random.fold_in(rng, 6), axis_at), (shards_of,), jnp.float32, smallest / len(split), largest / len(split))
        level = level * jnp.repeat(jnp.exp(heights), shape[axis_at] // shards_of).reshape((-1,) + (1,) * (len(shape) - 1 - axis_at))
    return level


def scatter_about(rng, extent, deviation, most, pieces=(), kind=jnp.bfloat16):
    factor_of = shard_levels(rng, extent, pieces, -0.22, 0.18) if pieces else 1.0
    values = jax.random.normal(rng, extent, jnp.float32) * deviation * factor_of
    return jnp.minimum(jnp.maximum(values, -most), most).astype(kind)


def setup_inputs(seed: int = 0) -> dict:
    splits = jax.random.split(jax.random.key(seed), 13)
    tokens = draw_tokens(jax.random.fold_in(splits[12], 71), 0)
    norm_gain = jnp.clip(1.0 + 0.18 * jax.random.normal(splits[1], (D,), jnp.float32), 0.1, 1.9)
    w_pool_in = scatter_about(splits[2], (D, POOL), D ** -0.5, 0.09375, ((1, 4),))
    w_query = draw_w_query(jax.random.fold_in(splits[12], 71), 0)
    w_key = draw_w_key(jax.random.fold_in(splits[12], 71), 0)
    w_value = scatter_about(splits[5], (D, HEADS * VDIM), D ** -0.5, 0.09375, ((1, 4),))
    pool_mix = scatter_about(splits[6], (GROUPS, GDIM, GDIM), GDIM ** -0.5, 0.75, ((0, 4),))
    pool_scale = jnp.clip(1.0 + 0.18 * jax.random.normal(splits[7], (POOL,), jnp.float32), 0.1, 1.9)
    lam = jnp.clip(0.3 + 0.5 * jax.random.uniform(splits[8], (HEADS,), jnp.float32) ** shard_levels(splits[8], (HEADS,), ((0, 4),), -0.2, 0.2), 0.3, 0.8)
    head_gain = jnp.clip(1.0 + 0.18 * jax.random.normal(splits[9], (VDIM,), jnp.float32), 0.1, 1.9)
    pool_proj = scatter_about(splits[10], (POOL, D), POOL ** -0.5, 0.125, ((0, 4),))
    attn_proj = scatter_about(splits[11], (HEADS * VDIM, D), (HEADS * VDIM) ** -0.5, 0.125, ((0, 4),))
    return {"tokens": tokens, "norm_gain": norm_gain, "w_pool_in": w_pool_in, "w_query": w_query, "w_key": w_key, "w_value": w_value, "pool_mix": pool_mix, "pool_scale": pool_scale, "lam": lam, "head_gain": head_gain, "pool_proj": pool_proj, "attn_proj": attn_proj}


eps_norm = 1e-06
neg_big = -1e+30
out_scale = 0.8

def reference(tokens, norm_gain, w_pool_in, w_query, w_key, w_value, pool_mix, pool_scale, lam, head_gain, pool_proj, attn_proj):
    wide = tokens.astype(jnp.float32)
    normed = (wide * lax.rsqrt(lax.optimization_barrier(jnp.mean(wide * wide, axis=-1, keepdims=True)) + eps_norm) * norm_gain).astype(jnp.bfloat16)
    pool_in = jnp.dot(normed, w_pool_in, preferred_element_type=jnp.float32).astype(jnp.bfloat16)
    query = jnp.dot(normed, w_query, preferred_element_type=jnp.float32).astype(jnp.bfloat16)
    keys = jnp.dot(normed, w_key, preferred_element_type=jnp.float32).astype(jnp.bfloat16)
    values = jnp.dot(normed, w_value, preferred_element_type=jnp.float32).astype(jnp.bfloat16)
    padded = jnp.concatenate([jnp.zeros((REACH - 1, POOL), jnp.float32), pool_in.astype(jnp.float32)], 0)
    channel_group = jnp.arange(POOL, dtype=jnp.int32) // GDIM
    window = 2 ** (1 + channel_group % 4)
    total = jnp.zeros((TOKENS, POOL), jnp.float32)
    for back in range(REACH):
        low = REACH - 1 - back
        total = total + jnp.where(back < window[None, :], padded[low:low + TOKENS], 0.0)
    position = jnp.arange(TOKENS, dtype=jnp.int32)
    count = jnp.minimum(position[:, None] + 1, window[None, :]).astype(jnp.float32)
    pooled = (total / count - pool_in.astype(jnp.float32)).astype(jnp.bfloat16)
    grouped = jnp.einsum('sgi,gio->sgo', pooled.reshape(TOKENS, GROUPS, GDIM).astype(jnp.float32), pool_mix.astype(jnp.float32))
    pool_out = (grouped.reshape(TOKENS, POOL) * pool_scale).astype(jnp.bfloat16)
    query_heads = query.reshape(TOKENS, HEADS, 2, HEAD).transpose(1, 0, 2, 3)
    key_heads = keys.reshape(TOKENS, HEADS, 2, HEAD).transpose(1, 0, 2, 3)
    value_heads = values.reshape(TOKENS, HEADS, VDIM).transpose(1, 0, 2)
    segments = position // SEGMENT
    block = min(TOKENS, 512) if TOKENS % min(TOKENS, 512) == 0 else TOKENS
    scale = HEAD ** (-0.5)

    def one_head(args):
        query_head, key_head, value_head, lam_head = args

        def one_block(index):
            first = (index * block).astype(jnp.int32)
            query_block = lax.dynamic_slice_in_dim(query_head, first, block, 0)
            query_seg = (first + jnp.arange(block, dtype=jnp.int32)) // SEGMENT
            allowed = segments[None, :] <= query_seg[:, None]
            results = []
            for which in range(2):
                scores = jnp.dot(query_block[:, which], key_head[:, which].T, preferred_element_type=jnp.float32) * scale
                masked = jnp.where(allowed, scores, neg_big)
                top = lax.optimization_barrier(jnp.max(masked, axis=-1, keepdims=True))
                probs = jnp.where(allowed, jnp.exp(masked - top), 0.0)
                weighted = jnp.dot(probs.astype(jnp.bfloat16), value_head, preferred_element_type=jnp.float32)
                results.append(weighted / lax.optimization_barrier(jnp.sum(probs, axis=-1, keepdims=True)))
            blend = results[0] - lam_head * results[1]
            scaled = blend * lax.rsqrt(lax.optimization_barrier(jnp.mean(blend * blend, axis=-1, keepdims=True)) + eps_norm) * head_gain * out_scale
            return scaled.astype(jnp.bfloat16)
        return lax.map(one_block, jnp.arange(TOKENS // block, dtype=jnp.int32))
    per_head = lax.map(one_head, (query_heads, key_heads, value_heads, lam))
    attn_out = per_head.reshape(HEADS, TOKENS, VDIM).transpose(1, 0, 2).reshape(TOKENS, HEADS * VDIM)
    pool_share = POOL // N_TP
    attn_share = HEADS * VDIM // N_TP
    summed = jnp.zeros((TOKENS, D), jnp.float32)
    for part in range(N_TP):
        term = jnp.dot(pool_out[:, part * pool_share:(part + 1) * pool_share], pool_proj[part * pool_share:(part + 1) * pool_share], preferred_element_type=jnp.float32)
        term = term + jnp.dot(attn_out[:, part * attn_share:(part + 1) * attn_share], attn_proj[part * attn_share:(part + 1) * attn_share], preferred_element_type=jnp.float32)
        summed = summed + lax.optimization_barrier(term.astype(jnp.bfloat16)).astype(jnp.float32)
    return summed.astype(jnp.bfloat16)
```

```python
import functools

import jax
import jax.numpy as jnp
from jax import lax
from jax.experimental import pallas as pl
from jax.experimental.pallas import tpu as pltpu
from jax.sharding import PartitionSpec as P

GDIM = 64
HEAD = 64
VDIM = 128
SEGMENT = 64
REACH = 16
CHUNK = 256

eps_norm = 1e-06
neg_big = -1e30
out_scale = 0.8
log2_e = 1.4426950408889634


def normalize(rows_in, gain):
    wide = rows_in.astype(jnp.float32)
    scaled = wide * lax.rsqrt(jnp.mean(wide * wide, axis=-1, keepdims=True) + eps_norm) * gain
    return scaled.astype(jnp.bfloat16)


def pool_kernel(x_ref, rim_ref, mix_ref, scale_ref, out_ref):
    rows, width = x_ref.shape
    x = x_ref[...].astype(jnp.float32)
    padded = jnp.concatenate([rim_ref[...].astype(jnp.float32), x], 0)
    group = lax.axis_index("tp") * (width // GDIM) + lax.broadcasted_iota(
        jnp.int32, (1, width), 1
    ) // GDIM
    window = 2 << (group % 4)
    running = padded
    total = jnp.zeros_like(padded)
    for level in range(4):
        running = running + pltpu.roll(running, 1 << level, 0)
        total = jnp.where(group % 4 == level, running, total)
    position = lax.axis_index("sp") * rows + lax.broadcasted_iota(jnp.int32, (rows, 1), 0)
    count = jnp.minimum(position + 1, window).astype(jnp.float32)
    pooled = (total[REACH:] / count - x).astype(jnp.bfloat16)
    for pair in range(width // 128):
        cols = slice(pair * 128, pair * 128 + 128)
        mixed = jnp.dot(pooled[:, cols], mix_ref[pair], preferred_element_type=jnp.float32)
        out_ref[:, cols] = (mixed * scale_ref[:, cols]).astype(jnp.bfloat16)


def pooling(pool_in, rim, pool_mix, pool_scale):
    groups = pool_mix.shape[0]
    pairs = pool_mix.reshape(groups // 2, 2, GDIM, GDIM)
    zero = jnp.zeros_like(pairs[:, 0])
    mix = jnp.concatenate(
        [
            jnp.concatenate([pairs[:, 0], zero], 2),
            jnp.concatenate([zero, pairs[:, 1]], 2),
        ],
        1,
    )
    rows, width = pool_in.shape
    return pl.pallas_call(
        pool_kernel,
        out_shape=jax.ShapeDtypeStruct((rows, width), jnp.bfloat16),
        cost_estimate=pl.CostEstimate(
            flops=rows * width * 256, bytes_accessed=4 * rows * width, transcendentals=0
        ),
        name="pooling",
    )(pool_in, rim, mix, pool_scale.reshape(1, width))


def attend_kernel(lam_ref, q_ref, k_ref, v_ref, gain_ref, out_ref, stacked, peak, total, acc):
    rows = q_ref.shape[0]
    head = pl.program_id(0)
    mine = lax.axis_index("sp")
    query = q_ref[...]
    lane = lax.broadcasted_iota(jnp.int32, query.shape, 1)
    stacked[:rows] = jnp.where(lane < HEAD, query, 0)
    stacked[rows:] = jnp.where(lane < HEAD, 0, query)

    def block(index, first):
        k = k_ref[pl.ds(pl.multiple_of(index * rows, rows), rows), :]
        v = v_ref[index]
        for start in range(0, 2 * rows, CHUNK):
            cols = slice(start, start + CHUNK)
            scores = lax.dot_general(
                k, stacked[cols], (((1,), (1,)), ((), ())), preferred_element_type=jnp.float32
            )
            if first:
                key_seg = lax.broadcasted_iota(jnp.int32, (rows, 1), 0) // SEGMENT
                query_seg = (
                    start % rows + lax.broadcasted_iota(jnp.int32, (1, CHUNK), 1)
                ) // SEGMENT
                scores = jnp.where(key_seg <= query_seg, scores, neg_big)
                top = jnp.max(scores, axis=0, keepdims=True)
            else:
                old = peak[:, cols]
                top = jnp.maximum(old, jnp.max(scores, axis=0, keepdims=True))
                shrink = jnp.exp2(old - top)
            probs = jnp.exp2(scores - top)
            summed = jnp.sum(probs, axis=0, keepdims=True)
            weighted = jnp.dot(v, probs.astype(jnp.bfloat16), preferred_element_type=jnp.float32)
            peak[:, cols] = top
            if first:
                total[:, cols] = summed
                acc[:, cols] = weighted
            else:
                total[:, cols] = total[:, cols] * shrink + summed
                acc[:, cols] = acc[:, cols] * shrink + weighted

    block(mine, True)

    @pl.loop(0, mine)
    def _(index):
        block(index, False)

    averaged = acc[...] / total[...]
    blend = averaged[:, :rows] - lam_ref[head] * averaged[:, rows:]
    scaled = blend * lax.rsqrt(jnp.mean(blend * blend, axis=0, keepdims=True) + eps_norm)
    out_ref[...] = (scaled.T * gain_ref[...] * out_scale).astype(jnp.bfloat16)


def attend(query, keys, values, lam, head_gain):
    rows, width = query.shape
    heads = width // VDIM
    parts, tokens = values.shape[0], keys.shape[0]
    work = rows * tokens * heads
    return pl.pallas_call(
        attend_kernel,
        grid=(heads,),
        in_specs=[
            pl.BlockSpec(memory_space=pltpu.SMEM),
            pl.BlockSpec((rows, VDIM), lambda h: (0, h)),
            pl.BlockSpec((tokens, VDIM), lambda h: (0, h)),
            pl.BlockSpec((parts, VDIM, rows), lambda h: (0, h, 0)),
            pl.BlockSpec((1, VDIM), lambda h: (0, 0)),
        ],
        out_specs=pl.BlockSpec((rows, VDIM), lambda h: (0, h)),
        out_shape=jax.ShapeDtypeStruct((rows, width), jnp.bfloat16),
        scratch_shapes=[
            pltpu.VMEM((2 * rows, VDIM), jnp.bfloat16),
            pltpu.VMEM((1, 2 * rows), jnp.float32),
            pltpu.VMEM((1, 2 * rows), jnp.float32),
            pltpu.VMEM((VDIM, 2 * rows), jnp.float32),
        ],
        cost_estimate=pl.CostEstimate(
            flops=work * 1024, bytes_accessed=4 * tokens * width, transcendentals=2 * work
        ),
        compiler_params=pltpu.CompilerParams(vmem_limit_bytes=48 * 2**20),
        name="attend",
    )(lam, query, keys, values, head_gain.reshape(1, VDIM))


def body(
    tokens,
    norm_gain,
    w_pool_in,
    w_query,
    w_key,
    w_value,
    pool_mix,
    pool_scale,
    lam,
    head_gain,
    pool_proj,
    attn_proj,
):
    count_rows = tokens.shape[0]
    normed = normalize(tokens, norm_gain)
    keys = jnp.dot(normed, w_key, preferred_element_type=jnp.float32).astype(jnp.bfloat16)
    all_keys = lax.all_gather(keys, "sp", axis=0, tiled=True)
    values = lax.dot_general(
        w_value, normed, (((0,), (1,)), ((), ())), preferred_element_type=jnp.float32
    ).astype(jnp.bfloat16)
    all_values = lax.all_gather(values, "sp", axis=0, tiled=False)
    pool_in = jnp.dot(normed, w_pool_in, preferred_element_type=jnp.float32).astype(jnp.bfloat16)
    devices = lax.axis_size("sp")
    rim = lax.ppermute(
        pool_in[count_rows - REACH :], "sp", [(i, i + 1) for i in range(devices - 1)]
    )
    query = (
        jnp.dot(normed, w_query, preferred_element_type=jnp.float32) * (HEAD ** (-0.5) * log2_e)
    ).astype(jnp.bfloat16)
    pool_out = pooling(pool_in, rim, pool_mix, pool_scale)
    attn_out = attend(query, all_keys, all_values, lam, head_gain)
    term = jnp.dot(pool_out, pool_proj, preferred_element_type=jnp.float32)
    return lax.psum_scatter(
        (term + jnp.dot(attn_out, attn_proj, preferred_element_type=jnp.float32)).astype(
            jnp.bfloat16
        ),
        "tp",
        scatter_dimension=0,
        tiled=True,
    )


def solution(mesh):
    return jax.shard_map(
        body,
        mesh=mesh,
        in_specs=(
            P("sp", None),
            P(),
            P(None, "tp"),
            P(None, "tp"),
            P(None, "tp"),
            P(None, "tp"),
            P("tp", None, None),
            P("tp"),
            P("tp"),
            P(),
            P("tp", None),
            P("tp", None),
        ),
        out_specs=P(("sp", "tp"), None),
        check_vma=False,
    )
```

```python
import functools

import jax
import jax.numpy as jnp
from jax import lax
from jax.experimental import pallas as pl
from jax.experimental.pallas import tpu as pltpu
from jax.sharding import PartitionSpec as P

GDIM = 64
HEAD = 64
VDIM = 128
SEGMENT = 64
REACH = 16
CHUNK = 256

eps_norm = 1e-06
neg_big = -1e30
out_scale = 0.8
log2_e = 1.4426950408889634


def normalize(rows_in, gain):
    wide = rows_in.astype(jnp.float32)
    scaled = wide * lax.rsqrt(jnp.mean(wide * wide, axis=-1, keepdims=True) + eps_norm) * gain
    return scaled.astype(jnp.bfloat16)


def pool_kernel(x_ref, rim_ref, mix_ref, scale_ref, out_ref):
    rows, width = x_ref.shape
    x = x_ref[...].astype(jnp.float32)
    padded = jnp.concatenate([rim_ref[...].astype(jnp.float32), x], 0)
    group = lax.axis_index("tp") * (width // GDIM) + lax.broadcasted_iota(
        jnp.int32, (1, width), 1
    ) // GDIM
    window = 2 << (group % 4)
    running = padded
    total = jnp.zeros_like(padded)
    for level in range(4):
        running = running + pltpu.roll(running, 1 << level, 0)
        total = jnp.where(group % 4 == level, running, total)
    position = lax.axis_index("sp") * rows + lax.broadcasted_iota(jnp.int32, (rows, 1), 0)
    count = jnp.minimum(position + 1, window).astype(jnp.float32)
    pooled = (total[REACH:] / count - x).astype(jnp.bfloat16)
    for pair in range(width // 128):
        cols = slice(pair * 128, pair * 128 + 128)
        mixed = jnp.dot(pooled[:, cols], mix_ref[pair], preferred_element_type=jnp.float32)
        out_ref[:, cols] = (mixed * scale_ref[:, cols]).astype(jnp.bfloat16)


def pooling(pool_in, rim, pool_mix, pool_scale):
    groups = pool_mix.shape[0]
    pairs = pool_mix.reshape(groups // 2, 2, GDIM, GDIM)
    zero = jnp.zeros_like(pairs[:, 0])
    mix = jnp.concatenate(
        [
            jnp.concatenate([pairs[:, 0], zero], 2),
            jnp.concatenate([zero, pairs[:, 1]], 2),
        ],
        1,
    )
    rows, width = pool_in.shape
    return pl.pallas_call(
        pool_kernel,
        out_shape=jax.ShapeDtypeStruct((rows, width), jnp.bfloat16),
        cost_estimate=pl.CostEstimate(
            flops=rows * width * 256, bytes_accessed=4 * rows * width, transcendentals=0
        ),
        name="pooling",
    )(pool_in, rim, mix, pool_scale.reshape(1, width))


def attend_kernel(lam_ref, all_ref, gain_ref, out_ref, turned, stacked, peak, total, acc):
    parts = all_ref.shape[0]
    sub = out_ref.shape[1]
    rows = (all_ref.shape[1] - sub) // 2
    chunk = min(CHUNK, 2 * sub)
    step = pl.program_id(0)
    share = rows // sub
    mine = lax.axis_index("sp")
    head, place = mine // share, mine % share

    @pl.when(step == 0)
    def _():
        @pl.loop(0, parts)
        def _(index):
            turned[index] = all_ref[index, rows : 2 * rows, :].T

    query = all_ref[step, 2 * rows :, :]
    lane = lax.broadcasted_iota(jnp.int32, query.shape, 1)
    stacked[:sub] = jnp.where(lane < HEAD, query, 0)
    stacked[sub:] = jnp.where(lane < HEAD, 0, query)

    def block(index, first):
        k = all_ref[index, :rows, :]
        v = turned[index]
        for start in range(0, 2 * sub, chunk):
            cols = slice(start, start + chunk)
            scores = lax.dot_general(
                k, stacked[cols], (((1,), (1,)), ((), ())), preferred_element_type=jnp.float32
            )
            if first:
                key_seg = lax.broadcasted_iota(jnp.int32, (rows, 1), 0) // SEGMENT
                query_at = (start + lax.broadcasted_iota(jnp.int32, (1, chunk), 1)) % sub
                query_seg = (place * sub + query_at) // SEGMENT
                scores = jnp.where(key_seg <= query_seg, scores, neg_big)
                top = jnp.max(scores, axis=0, keepdims=True)
            else:
                old = peak[:, cols]
                top = jnp.maximum(old, jnp.max(scores, axis=0, keepdims=True))
                shrink = jnp.exp2(old - top)
            probs = jnp.exp2(scores - top)
            summed = jnp.sum(probs, axis=0, keepdims=True)
            weighted = jnp.dot(v, probs.astype(jnp.bfloat16), preferred_element_type=jnp.float32)
            peak[:, cols] = top
            if first:
                total[:, cols] = summed
                acc[:, cols] = weighted
            else:
                total[:, cols] = total[:, cols] * shrink + summed
                acc[:, cols] = acc[:, cols] * shrink + weighted

    block(step, True)

    @pl.loop(0, step)
    def _(index):
        block(index, False)

    averaged = acc[...] / total[...]
    blend = averaged[:, :sub] - lam_ref[head] * averaged[:, sub:]
    scaled = blend * lax.rsqrt(jnp.mean(blend * blend, axis=0, keepdims=True) + eps_norm)
    out_ref[0] = (scaled.T * gain_ref[...] * out_scale).astype(jnp.bfloat16)


def attend(query, keys, values, lam, head_gain):
    rows, width = query.shape
    heads = width // VDIM
    parts = lax.axis_size("sp")
    share = parts // heads
    sub = rows // share

    def to_all(array):
        by_head = array.reshape(rows, heads, VDIM).transpose(1, 0, 2)
        return jnp.broadcast_to(by_head[:, None], (heads, share, rows, VDIM))

    query = query.reshape(share, sub, heads, VDIM).transpose(2, 0, 1, 3)
    sent = jnp.concatenate([to_all(keys), to_all(values), query], 2)
    sent = sent.reshape(parts, 2 * rows + sub, VDIM)
    received = lax.all_to_all(sent, "sp", 0, 0, tiled=True)
    work = rows * rows * parts * parts // share
    out = pl.pallas_call(
        attend_kernel,
        grid=(parts,),
        in_specs=[
            pl.BlockSpec(memory_space=pltpu.SMEM),
            pl.BlockSpec(received.shape, lambda i: (0, 0, 0)),
            pl.BlockSpec((1, VDIM), lambda i: (0, 0)),
        ],
        out_specs=pl.BlockSpec((1, sub, VDIM), lambda i: (i, 0, 0)),
        out_shape=jax.ShapeDtypeStruct((parts, sub, VDIM), jnp.bfloat16),
        scratch_shapes=[
            pltpu.VMEM((parts, VDIM, rows), jnp.bfloat16),
            pltpu.VMEM((2 * sub, VDIM), jnp.bfloat16),
            pltpu.VMEM((1, 2 * sub), jnp.float32),
            pltpu.VMEM((1, 2 * sub), jnp.float32),
            pltpu.VMEM((VDIM, 2 * sub), jnp.float32),
        ],
        cost_estimate=pl.CostEstimate(
            flops=work * 512, bytes_accessed=2 * received.size, transcendentals=work
        ),
        compiler_params=pltpu.CompilerParams(vmem_limit_bytes=40 * 2**20),
        name="attend",
    )(lam, received, head_gain.reshape(1, VDIM))
    back = lax.all_to_all(out, "sp", 0, 0, tiled=True)
    back = back.reshape(heads, share, sub, VDIM).transpose(1, 2, 0, 3)
    return back.reshape(rows, width)


def scatter_sum(term):
    devices = lax.axis_size("tp")
    pairs = [[i, i + 1] for i in range(0, devices, 2)]
    across = [list(range(core, devices, 2)) for core in range(2)]
    half = lax.psum_scatter(
        term, "tp", scatter_dimension=0, axis_index_groups=pairs, tiled=True
    )
    return lax.psum_scatter(
        half, "tp", scatter_dimension=0, axis_index_groups=across, tiled=True
    )


def by_core(array):
    devices = lax.axis_size("tp")
    rows, width = array.shape
    split = array.reshape(devices // 2, 2, rows // devices, width)
    return split.transpose(1, 0, 2, 3).reshape(rows, width)


def body(
    tokens,
    norm_gain,
    w_pool_in,
    w_query,
    w_key,
    w_value,
    pool_mix,
    pool_scale,
    lam,
    head_gain,
    pool_proj,
    attn_proj,
):
    count_rows = tokens.shape[0]
    normed = normalize(tokens, norm_gain)
    keys = jnp.dot(normed, w_key, preferred_element_type=jnp.float32).astype(jnp.bfloat16)
    values = jnp.dot(normed, w_value, preferred_element_type=jnp.float32).astype(jnp.bfloat16)
    pool_in = jnp.dot(normed, w_pool_in, preferred_element_type=jnp.float32).astype(jnp.bfloat16)
    devices = lax.axis_size("sp")
    rim = lax.ppermute(
        pool_in[count_rows - REACH :], "sp", [(i, i + 1) for i in range(devices - 1)]
    )
    query = (
        jnp.dot(normed, w_query, preferred_element_type=jnp.float32) * (HEAD ** (-0.5) * log2_e)
    ).astype(jnp.bfloat16)
    pool_out = pooling(pool_in, rim, pool_mix, pool_scale)
    attn_out = attend(query, keys, values, lam, head_gain)
    term = jnp.dot(by_core(pool_out), pool_proj, preferred_element_type=jnp.float32)
    term = term + jnp.dot(by_core(attn_out), attn_proj, preferred_element_type=jnp.float32)
    return scatter_sum(term.astype(jnp.bfloat16))


def solution(mesh):
    return jax.shard_map(
        body,
        mesh=mesh,
        in_specs=(
            P("sp", None),
            P(),
            P(None, "tp"),
            P(None, "tp"),
            P(None, "tp"),
            P(None, "tp"),
            P("tp", None, None),
            P("tp"),
            P("tp"),
            P(),
            P("tp", None),
            P("tp", None),
        ),
        out_specs=P(("sp", "tp"), None),
        check_vma=False,
    )
```

```python
import functools

import jax
import jax.numpy as jnp
from jax import lax
from jax.experimental import pallas as pl
from jax.experimental.pallas import tpu as pltpu
from jax.sharding import PartitionSpec as P

GDIM = 64
HEAD = 64
VDIM = 128
SEGMENT = 64
REACH = 16
CHUNK = 256

eps_norm = 1e-06
neg_big = -1e30
out_scale = 0.8
log2_e = 1.4426950408889634


def normalize(rows_in, gain):
    wide = rows_in.astype(jnp.float32)
    scaled = wide * lax.rsqrt(jnp.mean(wide * wide, axis=-1, keepdims=True) + eps_norm) * gain
    return scaled.astype(jnp.bfloat16)


def pool_kernel(x_ref, rim_ref, mix_ref, scale_ref, out_ref):
    rows, width = x_ref.shape
    x = x_ref[...].astype(jnp.float32)
    padded = jnp.concatenate([rim_ref[...].astype(jnp.float32), x], 0)
    group = lax.axis_index("tp") * (width // GDIM) + lax.broadcasted_iota(
        jnp.int32, (1, width), 1
    ) // GDIM
    window = 2 << (group % 4)
    running = padded
    total = jnp.zeros_like(padded)
    for level in range(4):
        running = running + pltpu.roll(running, 1 << level, 0)
        total = jnp.where(group % 4 == level, running, total)
    position = lax.axis_index("sp") * rows + lax.broadcasted_iota(jnp.int32, (rows, 1), 0)
    count = jnp.minimum(position + 1, window).astype(jnp.float32)
    pooled = (total[REACH:] / count - x).astype(jnp.bfloat16)
    for pair in range(width // 128):
        cols = slice(pair * 128, pair * 128 + 128)
        mixed = jnp.dot(pooled[:, cols], mix_ref[pair], preferred_element_type=jnp.float32)
        out_ref[:, cols] = (mixed * scale_ref[:, cols]).astype(jnp.bfloat16)


def pooling(pool_in, rim, pool_mix, pool_scale):
    groups = pool_mix.shape[0]
    pairs = pool_mix.reshape(groups // 2, 2, GDIM, GDIM)
    zero = jnp.zeros_like(pairs[:, 0])
    mix = jnp.concatenate(
        [
            jnp.concatenate([pairs[:, 0], zero], 2),
            jnp.concatenate([zero, pairs[:, 1]], 2),
        ],
        1,
    )
    rows, width = pool_in.shape
    return pl.pallas_call(
        pool_kernel,
        out_shape=jax.ShapeDtypeStruct((rows, width), jnp.bfloat16),
        cost_estimate=pl.CostEstimate(
            flops=rows * width * 256, bytes_accessed=4 * rows * width, transcendentals=0
        ),
        name="pooling",
    )(pool_in, rim, mix, pool_scale.reshape(1, width))


def attend_kernel(lam_ref, k_ref, v_ref, q_ref, gain_ref, out_ref, turned, stacked, peak, total, acc):
    parts, rows = k_ref.shape[:2]
    sub = out_ref.shape[1]
    chunk = min(CHUNK, 2 * sub)
    step = pl.program_id(0)
    share = rows // sub
    mine = lax.axis_index("sp")
    head, place = mine // share, mine % share

    @pl.when(step == 0)
    def _():
        @pl.loop(0, parts)
        def _(index):
            turned[index] = v_ref[index].T

    query = q_ref[step]
    lane = lax.broadcasted_iota(jnp.int32, query.shape, 1)
    stacked[:sub] = jnp.where(lane < HEAD, query, 0)
    stacked[sub:] = jnp.where(lane < HEAD, 0, query)

    def block(index, first):
        k = k_ref[index]
        v = turned[index]
        for start in range(0, 2 * sub, chunk):
            cols = slice(start, start + chunk)
            scores = lax.dot_general(
                k, stacked[cols], (((1,), (1,)), ((), ())), preferred_element_type=jnp.float32
            )
            if first:
                key_seg = lax.broadcasted_iota(jnp.int32, (rows, 1), 0) // SEGMENT
                query_at = (start + lax.broadcasted_iota(jnp.int32, (1, chunk), 1)) % sub
                query_seg = (place * sub + query_at) // SEGMENT
                scores = jnp.where(key_seg <= query_seg, scores, neg_big)
                top = jnp.max(scores, axis=0, keepdims=True)
            else:
                old = peak[:, cols]
                top = jnp.maximum(old, jnp.max(scores, axis=0, keepdims=True))
                shrink = jnp.exp2(old - top)
            probs = jnp.exp2(scores - top)
            summed = jnp.sum(probs, axis=0, keepdims=True)
            weighted = jnp.dot(v, probs.astype(jnp.bfloat16), preferred_element_type=jnp.float32)
            peak[:, cols] = top
            if first:
                total[:, cols] = summed
                acc[:, cols] = weighted
            else:
                total[:, cols] = total[:, cols] * shrink + summed
                acc[:, cols] = acc[:, cols] * shrink + weighted

    block(step, True)

    @pl.loop(0, step)
    def _(index):
        block(index, False)

    averaged = acc[...] / total[...]
    blend = averaged[:, :sub] - lam_ref[head] * averaged[:, sub:]
    scaled = blend * lax.rsqrt(jnp.mean(blend * blend, axis=0, keepdims=True) + eps_norm)
    out_ref[0] = (scaled.T * gain_ref[...] * out_scale).astype(jnp.bfloat16)


def attend(query, keys, values, lam, head_gain):
    rows, width = query.shape
    heads = width // VDIM
    parts = lax.axis_size("sp")
    share = parts // heads
    sub = rows // share

    def to_all(array):
        by_head = array.reshape(rows, heads, VDIM).transpose(1, 0, 2)
        copies = jnp.broadcast_to(by_head[:, None], (heads, share, rows, VDIM))
        copies = copies.reshape(parts, rows, VDIM)
        return lax.all_to_all(copies, "sp", 0, 0, tiled=True)

    query = query.reshape(share, sub, heads, VDIM).transpose(2, 0, 1, 3)
    query = query.reshape(parts, sub, VDIM)
    received = (
        to_all(keys),
        to_all(values),
        lax.all_to_all(query, "sp", 0, 0, tiled=True),
    )
    work = rows * rows * parts * parts // share
    out = pl.pallas_call(
        attend_kernel,
        grid=(parts,),
        in_specs=[
            pl.BlockSpec(memory_space=pltpu.SMEM),
            *[pl.BlockSpec(array.shape, lambda i: (0, 0, 0)) for array in received],
            pl.BlockSpec((1, VDIM), lambda i: (0, 0)),
        ],
        out_specs=pl.BlockSpec((1, sub, VDIM), lambda i: (i, 0, 0)),
        out_shape=jax.ShapeDtypeStruct((parts, sub, VDIM), jnp.bfloat16),
        scratch_shapes=[
            pltpu.VMEM((parts, VDIM, rows), jnp.bfloat16),
            pltpu.VMEM((2 * sub, VDIM), jnp.bfloat16),
            pltpu.VMEM((1, 2 * sub), jnp.float32),
            pltpu.VMEM((1, 2 * sub), jnp.float32),
            pltpu.VMEM((VDIM, 2 * sub), jnp.float32),
        ],
        cost_estimate=pl.CostEstimate(
            flops=work * 512, bytes_accessed=6 * received[0].size, transcendentals=work
        ),
        compiler_params=pltpu.CompilerParams(vmem_limit_bytes=40 * 2**20),
        name="attend",
    )(lam, *received, head_gain.reshape(1, VDIM))
    back = lax.all_to_all(out, "sp", 0, 0, tiled=True)
    back = back.reshape(heads, share, sub, VDIM).transpose(1, 2, 0, 3)
    return back.reshape(rows, width)


def body(
    tokens,
    norm_gain,
    w_pool_in,
    w_query,
    w_key,
    w_value,
    pool_mix,
    pool_scale,
    lam,
    head_gain,
    pool_proj,
    attn_proj,
):
    count_rows = tokens.shape[0]
    normed = normalize(tokens, norm_gain)
    keys = jnp.dot(normed, w_key, preferred_element_type=jnp.float32).astype(jnp.bfloat16)
    values = jnp.dot(normed, w_value, preferred_element_type=jnp.float32).astype(jnp.bfloat16)
    pool_in = jnp.dot(normed, w_pool_in, preferred_element_type=jnp.float32).astype(jnp.bfloat16)
    devices = lax.axis_size("sp")
    rim = lax.ppermute(
        pool_in[count_rows - REACH :], "sp", [(i, i + 1) for i in range(devices - 1)]
    )
    query = (
        jnp.dot(normed, w_query, preferred_element_type=jnp.float32) * (HEAD ** (-0.5) * log2_e)
    ).astype(jnp.bfloat16)
    pool_out = pooling(pool_in, rim, pool_mix, pool_scale)
    attn_out = attend(query, keys, values, lam, head_gain)
    term = jnp.dot(pool_out, pool_proj, preferred_element_type=jnp.float32)
    term = term + jnp.dot(attn_out, attn_proj, preferred_element_type=jnp.float32)
    return lax.psum_scatter(
        term.astype(jnp.bfloat16), "tp", scatter_dimension=0, tiled=True
    )


def solution(mesh):
    return jax.shard_map(
        body,
        mesh=mesh,
        in_specs=(
            P("sp", None),
            P(),
            P(None, "tp"),
            P(None, "tp"),
            P(None, "tp"),
            P(None, "tp"),
            P("tp", None, None),
            P("tp"),
            P("tp"),
            P(),
            P("tp", None),
            P("tp", None),
        ),
        out_specs=P(("sp", "tp"), None),
        check_vma=False,
    )
```
